32 devices in a mesh: grp: 2 (over y), ep: 4 (over z), tp: 4 (over x, core).
Axes of the slice: x: 2, y: 2, z: 4, core: 2. Of those that a mesh axis runs over, the one named last changes fastest.
Arguments:
- query_first: bfloat16 [3072, 512], P(('grp', 'ep'), 'tp'), parts along dimension 0, may hold values from -32 to 32
- query_second: bfloat16 [3072, 512], P(('grp', 'ep'), 'tp'), parts along dimension 0, may hold values from -32 to 32
- key_first: bfloat16 [3072, 512], P(('grp', 'ep'), 'tp'), parts along dimension 0, may hold values from -32 to 32
- key_second: bfloat16 [3072, 512], P(('grp', 'ep'), 'tp'), parts along dimension 0, may hold values from -32 to 32
- values: bfloat16 [3072, 1024], P(('grp', 'ep'), 'tp'), parts along dimension 0, may hold values from -6 to 6
- lambda_head: float32 [8], P('tp'), may hold values from 0.3 to 0.8
- head_gain: float32 [128], replicated, may hold values from 0.1 to 1.9
- out_weight: bfloat16 [1024, 2048], replicated, may hold values from -0.1875 to 0.1875
- tokens: bfloat16 [4096, 2048], P(('grp', 'ep', 'tp')), parts along dimension 0, may hold values from -6 to 6
- norm_gain: float32 [2048], replicated, may hold values from 0.1 to 1.9
- expert_ids: int32 [4096, 2], P(('grp', 'ep', 'tp')), parts along dimension 0, may hold values from 0 to 3, all different within a row; in each aligned block of 128 rows (0 to 127, 128 to 255, ...) at most 96 rows name the same one
- expert_weights: float32 [4096, 2], P(('grp', 'ep', 'tp')), parts along dimension 0, may hold values from 0.2 to 1
- expert_gate: bfloat16 [4, 2048, 1024], P('ep', None, 'tp'), may hold values from -0.125 to 0.125
- expert_up: bfloat16 [4, 2048, 1024], P('ep', None, 'tp'), may hold values from -0.125 to 0.125
- expert_down: bfloat16 [4, 1024, 2048], P('ep', 'tp'), may hold values from -0.1875 to 0.1875
- shared_gate: bfloat16 [2048, 512], P(None, 'tp'), may hold values from -0.125 to 0.125
- shared_up: bfloat16 [2048, 512], P(None, 'tp'), may hold values from -0.125 to 0.125
- shared_down: bfloat16 [512, 2048], P('tp'), may hold values from -0.25 to 0.25
Outputs:
- mixed: bfloat16 [3072, 2048], P(('grp', 'ep', 'tp')), parts along dimension 0
- expert_out: bfloat16 [4096, 2048], P(('grp', 'ep', 'tp')), parts along dimension 0
The draws below stay inside these ranges and needn't reach their ends.
There are 2 independent parts, one for each index of `grp`. The reference program is written for one: setup_inputs(seed, part) draws one part's arguments, and reference() takes and returns one part's arrays. A program takes and returns all parts, laid end to end along the dimension named above; an argument that names none is the same for every part. Nothing has to cross between parts.
Inputs may be any that keep to these rules, and one draw needn't show every extreme that they name: `expert_ids`: in the rows of one device (aligned blocks of 128 rows) no expert is named by more than 96 rows, and in every draw some expert is named by exactly 96 rows of some block; each row names 2 different experts.
All inputs are finite; a program needn't handle non-finite values.
Results may differ from the reference program's by a relative error of at most 0.012.
Values may be sent and summed in bfloat16 or wider, within the bound.
No kernel may reach another device: no remote copies, remote signals or barrier semaphores. Data moves between devices by JAX's collectives and lax.ppermute only.
A program may use at most 128 MiB of HBM per device.

```python
import math
import jax
import jax.numpy as jnp
import numpy as np
from jax import lax

D = 2048
HEADS = 8
HEAD = 64
VDIM = 128
FF = 1024
SHARED = 512
TOPK = 2
ROW_DEV = 128
TOKENS_A = 1536
TOKENS_E = 2048
EXPERTS = 4
CAP = 96
N_TP = 4


def drawn_pair(key, which):
    base = jax.random.fold_in(key, 4100 + which)
    key_query, key_keys = jax.random.split(base, 2)
    shape = (TOKENS_A, HEADS * HEAD)
    queries = 1.3 * jax.random.truncated_normal(key_query, -3.8, 3.8, shape, jnp.float32)
    keys = 1.3 * jax.random.truncated_normal(key_keys, -3.8, 3.8, shape, jnp.float32)
    return (queries.astype(jnp.bfloat16), keys.astype(jnp.bfloat16))


def draw_query_first(key, part):
    return drawn_pair(key, 0)[0]


def draw_key_first(key, part):
    return drawn_pair(key, 0)[1]


def draw_query_second(key, part):
    return drawn_pair(key, 1)[0]


def draw_key_second(key, part):
    return drawn_pair(key, 1)[1]


def steps_of(key, dims, cuts, smallest, largest):
    level = 1.0
    for dim, parts in cuts:
        heights = jax.random.uniform(jax.random.fold_in(jax.random.fold_in(key, 6), dim), (parts,), jnp.float32, smallest / len(cuts), largest / len(cuts))
        level = level * jnp.repeat(jnp.exp(heights), dims[dim] // parts).reshape((-1,) + (1,) * (len(dims) - 1 - dim))
    return level


def deal_out(key, own, number, rows, number_of, top, bound, slope):
    sequence = jax.random.permutation(key, number_of)
    heavy_load, ordinary = portions_of(number_of, rows * top, bound, slope, True), portions_of(number_of, rows * top, bound, slope, False)
    places = jnp.arange(number_of)

    def named(lengths, turn):
        used = int((lengths > 0).sum())
        fixed = max(1, used // 4)
        shifted = fixed + (places - fixed + turn * (used - fixed)) % max(1, number_of - fixed)
        return jnp.zeros((number_of,), jnp.int32).at[sequence[jnp.where(places < fixed, places, shifted)]].set(jnp.asarray(lengths, jnp.int32))

    lengths = jnp.where(number % 4 == 0, named(heavy_load, number // 4), named(ordinary, number - number // 4 - 1))
    mixed = jax.random.permutation(jax.random.fold_in(own, 3), number_of)
    donor, receiver = mixed[0:number_of // 2 * 2:2], mixed[1:number_of // 2 * 2:2]
    slack = jnp.minimum(lengths[donor] - 1, bound - lengths[receiver]) // 2
    slack = jnp.where((donor == sequence[0]) | (receiver == sequence[0]) | (lengths[receiver] == 0), 0, jnp.maximum(slack, 0))
    shifted = jax.random.randint(jax.random.fold_in(own, 4), (number_of // 2,), 0, 1 << 20) % (slack + 1)
    lengths = lengths.at[donor].add(-shifted).at[receiver].add(shifted)
    items = jnp.searchsorted(jnp.cumsum(lengths), jnp.arange(rows * top), side="right").astype(jnp.int32)
    grid = items.reshape(top, rows).T
    grid = grid[jax.random.permutation(jax.random.fold_in(own, 1), rows)]
    turn = jax.random.randint(jax.random.fold_in(own, 2), (rows, 1), 0, top)
    return jnp.take_along_axis(grid, (jnp.arange(top)[None, :] + turn) % top, axis=1)


def portions_of(number_of, total, most, skew, full):
    portions = [(1 << 20) // math.isqrt(rank ** skew) + 1 for rank in range(1, number_of + 1)]
    largest = most if full else min(most, max(-(-total // number_of), total * portions[0] // sum(portions)))
    least = 1 if total - largest >= number_of - 1 else 0
    counts, rest = [largest] + [least] * (number_of - 1), total - largest - least * (number_of - 1)
    while rest > 0:
        movable = [i for i in range(1, number_of) if counts[i] < largest] or [i for i in range(1, number_of) if counts[i] < most]
        whole, budget = sum([portions[i] for i in movable]), rest
        for i in movable:
            addition = min(most - counts[i], max(1, budget * portions[i] // whole), rest)
            counts[i] = counts[i] + addition
            rest = rest - addition
    return np.array(counts)


def centred(stream_key, shape, scale, limit, shards=(), held_as=jnp.bfloat16):
    drawn = jax.random.normal(stream_key, shape, jnp.float32) * scale
    if len(shards) > 0:
        drawn = steps_of(stream_key, shape, shards, -0.22, 0.18) * drawn
    return jnp.clip(drawn, min=-limit, max=limit).astype(held_as)


def setup_inputs(seed: int = 0, part: int = 0) -> dict:
    streams_of = jax.random.split(jax.random.key(seed), 19)
    part_keys = jax.random.split(jax.random.fold_in(streams_of[18], part), 19)
    query_first = draw_query_first(jax.random.fold_in(jax.random.fold_in(streams_of[18], part), 71), part)
    query_second = draw_query_second(jax.random.fold_in(jax.random.fold_in(streams_of[18], part), 71), part)
    key_first = draw_key_first(jax.random.fold_in(jax.random.fold_in(streams_of[18], part), 71), part)
    key_second = draw_key_second(jax.random.fold_in(jax.random.fold_in(streams_of[18], part), 71), part)
    values = centred(part_keys[4], (TOKENS_A, HEADS * VDIM), 1.0, 6.0, ((0, 4), (1, 4)))
    lambda_head = jnp.clip(0.3 + 0.5 * jax.random.uniform(streams_of[5], (HEADS,), jnp.float32) ** steps_of(streams_of[5], (HEADS,), ((0, 4),), -0.2, 0.2), 0.3, 0.8)
    head_gain = jnp.clip(1.0 + 0.18 * jax.random.normal(streams_of[6], (VDIM,), jnp.float32), 0.1, 1.9)
    out_weight = centred(streams_of[7], (HEADS * VDIM, D), (HEADS * VDIM) ** -0.5, 0.1875)
    tokens = centred(part_keys[8], (TOKENS_E, D), 1.0, 6.0, ((0, 16),))
    norm_gain = jnp.clip(1.0 + 0.18 * jax.random.normal(streams_of[9], (D,), jnp.float32), 0.1, 1.9)
    expert_ids_keys = jax.random.split(jax.random.fold_in(part_keys[10], 1), TOKENS_E // ROW_DEV)
    expert_ids_turns = jax.random.permutation(jax.random.fold_in(part_keys[10], 3), TOKENS_E // ROW_DEV)
    expert_ids = jax.vmap(lambda own, number: deal_out(jax.random.fold_in(part_keys[10], 2), own, number, ROW_DEV, EXPERTS, TOPK, CAP, 1))(expert_ids_keys, expert_ids_turns).reshape((TOKENS_E, TOPK))
    expert_weights = jnp.clip(0.2 + 0.8 * jax.random.uniform(part_keys[11], (TOKENS_E, TOPK), jnp.float32) ** steps_of(part_keys[11], (TOKENS_E, TOPK), ((0, 16),), -0.2, 0.2), 0.2, 1.0)
    expert_gate = centred(streams_of[12], (EXPERTS, D, FF), D ** -0.5, 0.125, ((0, 4), (2, 4)))
    expert_up = centred(streams_of[13], (EXPERTS, D, FF), D ** -0.5, 0.125, ((0, 4), (2, 4)))
    expert_down = centred(streams_of[14], (EXPERTS, FF, D), FF ** -0.5, 0.1875, ((0, 4), (1, 4)))
    shared_gate = centred(streams_of[15], (D, SHARED), D ** -0.5, 0.125, ((1, 4),))
    shared_up = centred(streams_of[16], (D, SHARED), D ** -0.5, 0.125, ((1, 4),))
    shared_down = centred(streams_of[17], (SHARED, D), SHARED ** -0.5, 0.25, ((0, 4),))
    return {"query_first": query_first, "query_second": query_second, "key_first": key_first, "key_second": key_second, "values": values, "lambda_head": lambda_head, "head_gain": head_gain, "out_weight": out_weight, "tokens": tokens, "norm_gain": norm_gain, "expert_ids": expert_ids, "expert_weights": expert_weights, "expert_gate": expert_gate, "expert_up": expert_up, "expert_down": expert_down, "shared_gate": shared_gate, "shared_up": shared_up, "shared_down": shared_down}


epsilon = 1e-06

def reference(query_first, query_second, key_first, key_second, values, lambda_head, head_gain, out_weight, tokens, norm_gain, expert_ids, expert_weights, expert_gate, expert_up, expert_down, shared_gate, shared_up, shared_down):
    score_scale = HEAD ** (-0.5)
    key_one = key_first.astype(jnp.float32).reshape(TOKENS_A, HEADS, HEAD)
    key_two = key_second.astype(jnp.float32).reshape(TOKENS_A, HEADS, HEAD)
    value_all = values.astype(jnp.float32).reshape(TOKENS_A, HEADS, VDIM)
    query_rows = math.gcd(TOKENS_A, 256)

    def one_map(queries, keys):
        scores = jnp.einsum('qhd,khd->qhk', queries, keys) * score_scale
        row_peak = lax.optimization_barrier(jnp.max(scores, axis=-1, keepdims=True))
        exponent = jnp.exp(scores - row_peak)
        row_total = lax.optimization_barrier(jnp.sum(exponent, axis=-1))
        rounded = lax.optimization_barrier(exponent.astype(jnp.bfloat16)).astype(jnp.float32)
        return jnp.einsum('qhk,khe->qhe', rounded, value_all) / row_total[..., None]

    def query_block(query_pair):
        first_block, second_block = query_pair
        mixture = one_map(first_block, key_one) - lambda_head[None, :, None] * one_map(second_block, key_two)
        normed_heads = mixture * lax.rsqrt(lax.optimization_barrier(jnp.mean(mixture * mixture, axis=-1, keepdims=True)) + epsilon) * head_gain
        return normed_heads.astype(jnp.bfloat16)
    query_one = query_first.astype(jnp.float32).reshape(TOKENS_A // query_rows, query_rows, HEADS, HEAD)
    query_two = query_second.astype(jnp.float32).reshape(TOKENS_A // query_rows, query_rows, HEADS, HEAD)
    head_rows = lax.map(query_block, (query_one, query_two)).reshape(TOKENS_A, HEADS * VDIM)
    mixed = jnp.dot(head_rows, out_weight, preferred_element_type=jnp.float32).astype(jnp.bfloat16)
    widened = tokens.astype(jnp.float32)
    normed = (widened * lax.rsqrt(lax.optimization_barrier(jnp.mean(widened * widened, axis=-1, keepdims=True)) + epsilon) * norm_gain).astype(jnp.bfloat16)
    block_count = TOKENS_E // ROW_DEV
    copies = ROW_DEV * TOPK
    chosen = expert_ids.reshape(block_count, copies)
    onehot = (chosen[:, :, None] == jnp.arange(EXPERTS, dtype=jnp.int32)[None, None, :]).astype(jnp.int32)
    rank_in_block = lax.optimization_barrier(jnp.sum(onehot * jnp.cumsum(onehot, axis=1), axis=-1)) - 1
    block_index = jnp.arange(block_count, dtype=jnp.int32)[:, None]
    slot_index = (chosen * (block_count * CAP) + block_index * CAP + rank_in_block).reshape(-1)
    token_index = (block_index * ROW_DEV + jnp.arange(copies, dtype=jnp.int32)[None, :] // TOPK).reshape(-1)
    slot_tokens = jnp.full((EXPERTS * block_count * CAP,), TOKENS_E, jnp.int32).at[slot_index].set(token_index)
    slot_tokens = slot_tokens.reshape(EXPERTS, block_count * CAP)
    slot_weights = jnp.zeros((EXPERTS * block_count * CAP,), jnp.float32).at[slot_index].set(expert_weights.reshape(-1))
    slot_weights = slot_weights.reshape(EXPERTS, block_count * CAP)
    padded = jnp.concatenate([normed, jnp.zeros((1, D), jnp.bfloat16)], axis=0)

    def expert_step(accum, inputs):
        index_rows, weight_rows, gate_matrix, up_matrix, down_matrix = inputs
        picked = padded[index_rows]
        gate_value = jnp.dot(picked, gate_matrix, preferred_element_type=jnp.float32)
        up_value = jnp.dot(picked, up_matrix, preferred_element_type=jnp.float32)
        hidden = (jax.nn.silu(gate_value) * up_value).astype(jnp.bfloat16)
        grouped = hidden.astype(jnp.float32).reshape(-1, N_TP, FF // N_TP)
        down_groups = down_matrix.astype(jnp.float32).reshape(N_TP, FF // N_TP, D)
        partial_value = jnp.einsum('mjf,jfd->jmd', grouped, down_groups)
        rounded = lax.optimization_barrier(partial_value.astype(jnp.bfloat16)).astype(jnp.float32)
        routed = lax.optimization_barrier(lax.optimization_barrier(jnp.sum(rounded, axis=0)).astype(jnp.bfloat16)).astype(jnp.float32)
        return (accum.at[index_rows].add(routed * weight_rows[:, None]), None)
    accum_start = jnp.zeros((TOKENS_E + 1, D), jnp.float32)
    routed_sum, unused = lax.scan(expert_step, accum_start, (slot_tokens, slot_weights, expert_gate, expert_up, expert_down))
    group_width = SHARED // N_TP
    shared_part = jnp.zeros((TOKENS_E, D), jnp.float32)
    for quarter in range(N_TP):
        columns = slice(quarter * group_width, (quarter + 1) * group_width)
        gate_value = jnp.dot(normed, shared_gate[:, columns], preferred_element_type=jnp.float32)
        up_value = jnp.dot(normed, shared_up[:, columns], preferred_element_type=jnp.float32)
        shared_hidden = (jax.nn.silu(gate_value) * up_value).astype(jnp.bfloat16)
        partial_value = jnp.dot(shared_hidden, shared_down[columns, :], preferred_element_type=jnp.float32)
        shared_part = shared_part + lax.optimization_barrier(partial_value.astype(jnp.bfloat16)).astype(jnp.float32)
    expert_out = (routed_sum[:TOKENS_E] + shared_part).astype(jnp.bfloat16)
    return (mixed, expert_out)
```

```python
import functools

import jax
import jax.numpy as jnp
from jax import lax
from jax.experimental import pallas as pl
from jax.experimental.pallas import tpu as pltpu
from jax.sharding import PartitionSpec as P

epsilon = 1e-06
block_limit = 1536
lane_count = 128
third = 32


def key_block(total_rows, shard_rows):
    if total_rows <= block_limit or total_rows % shard_rows != 0:
        return total_rows
    best_rows = shard_rows
    for factor_rows in range(1, total_rows // shard_rows + 1):
        if total_rows % (factor_rows * shard_rows) == 0 and factor_rows * shard_rows <= block_limit:
            best_rows = factor_rows * shard_rows
    return best_rows


def softmax_update(states, scores, value_block):
    running_max, running_sum, accumulated = states
    new_max = jnp.maximum(running_max, jnp.max(scores, axis=-1))
    rescale = jnp.exp(running_max - new_max)
    weights = jnp.exp(scores - new_max[..., None])
    new_sum = running_sum * rescale + jnp.sum(weights, axis=-1)
    product = jnp.einsum(
        "qhk,khe->qhe",
        weights.astype(jnp.bfloat16),
        value_block,
        preferred_element_type=jnp.float32,
    )
    return (new_max, new_sum, accumulated * rescale[..., None] + product)


def relay_pairs(count, width, step):
    upward = [(z * width + t, (z + 1) * width + t) for t in range(0, width, 2) for z in range(step - 1, count - 1)]
    downward = [(z * width + t, (z - 1) * width + t) for t in range(1, width, 2) for z in range(1, count - step + 1)]
    return upward + downward


def return_pairs(count, width, step):
    downward = [(z * width + t, (z - 1) * width + t) for t in range(0, width, 2) for z in range(count - step, count)]
    upward = [(z * width + t, (z + 1) * width + t) for t in range(1, width, 2) for z in range(step)]
    return downward + upward


def swap_core(value):
    return lax.ppermute(value, "tp", [(t, t ^ 1) for t in range(lax.axis_size("tp"))])


def swap_pair(value):
    return lax.ppermute(value, "tp", [(t, t ^ 2) for t in range(lax.axis_size("tp"))])


def swap_group(value):
    return lax.ppermute(value, "grp", [(0, 1), (1, 0)])


def silu(value):
    return value / (1.0 + jnp.exp(-value))


def prepare_body(own, other, route_own, route_other, gain, out):
    rows, width = own.shape
    for index, (block, route) in enumerate(((own, route_own), (other, route_other))):
        wide = block[...].astype(jnp.float32)
        scale = lax.rsqrt(jnp.mean(wide * wide, axis=-1, keepdims=True) + epsilon)
        out[pl.ds(index * rows, rows), pl.ds(0, width)] = (wide * scale * gain[...]).astype(jnp.bfloat16)
        lanes = lax.broadcasted_iota(jnp.int32, (rows, lane_count), 1)
        table = route[...]
        picks = table.shape[1] // 2
        part = jnp.zeros((rows, lane_count), jnp.float32)
        for pick in range(picks):
            chosen = table[:, pick : pick + 1].astype(jnp.int32)
            weight = table[:, picks + pick : picks + pick + 1]
            part = part + jnp.where((lanes & (third - 1)) == chosen, weight, 0.0)
        high = part.astype(jnp.bfloat16)
        rest = part - high.astype(jnp.float32)
        middle = rest.astype(jnp.bfloat16)
        low = (rest - middle.astype(jnp.float32)).astype(jnp.bfloat16)
        level = lanes // third
        mixed = jnp.where(
            level == 0,
            high.astype(jnp.float32),
            jnp.where(level == 1, middle.astype(jnp.float32), jnp.where(level == 2, low.astype(jnp.float32), 0.0)),
        )
        out[pl.ds(index * rows, rows), pl.ds(width, lane_count)] = mixed.astype(jnp.bfloat16)


def prepare(own, other, route_own, route_other, gain):
    rows, width = own.shape
    return pl.pallas_call(
        prepare_body,
        out_shape=jax.ShapeDtypeStruct((2 * rows, width + lane_count), jnp.bfloat16),
        cost_estimate=pl.CostEstimate(flops=8 * rows * width, bytes_accessed=8 * rows * width, transcendentals=rows),
        name="prepare",
    )(own, other, route_own, route_other, gain.reshape(1, width))


def halves_body(which, gate, up, out):
    half = gate.shape[1]
    out[:, pl.ds(0, half)] = gate[...]
    out[:, pl.ds(half, half)] = up[...]


def halves(gate, up, which):
    width, units = gate.shape
    rows = min(512, width)
    half = units // 2
    return pl.pallas_call(
        halves_body,
        grid_spec=pltpu.PrefetchScalarGridSpec(
            num_scalar_prefetch=1,
            grid=(width // rows,),
            in_specs=[
                pl.BlockSpec((rows, half), lambda i, which: (i, which[0])),
                pl.BlockSpec((rows, half), lambda i, which: (i, which[0])),
            ],
            out_specs=pl.BlockSpec((rows, units), lambda i, which: (i, 0)),
        ),
        out_shape=jax.ShapeDtypeStruct((width, units), jnp.bfloat16),
        cost_estimate=pl.CostEstimate(flops=width * units, bytes_accessed=4 * width * units, transcendentals=0),
        name="halves",
    )(which.reshape(1), gate, up)


def feed_forward_body(plan, block_count, weighted, *refs):
    blocks = refs[:block_count]
    mask = refs[block_count]
    weight_count = plan["weights"]
    weights = refs[block_count + 1 : block_count + 1 + weight_count]
    outs = refs[block_count + 1 + weight_count : 2 * block_count + 1 + weight_count]
    scratch = refs[2 * block_count + 1 + weight_count :]
    joined_buffer, down_buffer, hidden, sems = scratch
    width = plan["width"]
    copies = {}
    for number, (index, kind, start, size) in enumerate(plan["copies"]):
        if kind == "column":
            target = joined_buffer.at[start]
        else:
            target = down_buffer.at[pl.ds(start, size), :]
        copies[index] = pltpu.make_async_copy(weights[index], target, sems.at[number])
        copies[index].start()
    for piece in plan["pieces"]:
        for index in piece["needs"]:
            copies[index].wait()
        for number, block in enumerate(blocks):
            rows = block.shape[0]
            first_row = plan["rows"][number]
            x = block[:, pl.ds(0, width)]
            if piece["kind"] == "two":
                gate = jnp.dot(x, joined_buffer[piece["slots"][0]], preferred_element_type=jnp.float32)
                up = jnp.dot(x, joined_buffer[piece["slots"][1]], preferred_element_type=jnp.float32)
            else:
                both = jnp.dot(x, joined_buffer[piece["slots"][0]], preferred_element_type=jnp.float32)
                units = both.shape[1] // 2
                gate, up = both[:, :units], both[:, units:]
            hidden[pl.ds(first_row, rows), pl.ds(piece["start"], piece["units"])] = (silu(gate) * up).astype(
                jnp.bfloat16
            )
    for index in plan["downs"]:
        copies[index].wait()
    for number, block in enumerate(blocks):
        rows = block.shape[0]
        first_row = plan["rows"][number]
        result = jnp.dot(
            hidden[pl.ds(first_row, rows), :], down_buffer[...], preferred_element_type=jnp.float32
        )
        if weighted:
            table = block[:, pl.ds(width, lane_count)].astype(jnp.float32)
            result = result * jnp.sum(table * mask[...], axis=-1, keepdims=True)
        outs[number][...] = result.astype(outs[number].dtype)


def feed_forward(blocks, mask, pairs, joined, weighted, out_types, width, name):
    weights, copies, pieces, downs = [], [], [], []
    slot, start = 0, 0
    for gate, up, down in pairs:
        base = len(weights)
        weights += [gate, up, down]
        units = gate.shape[1]
        copies += [(base, "column", slot, 0), (base + 1, "column", slot + 1, 0), (base + 2, "row", start, units)]
        pieces.append({"kind": "two", "slots": (slot, slot + 1), "needs": (base, base + 1), "start": start, "units": units})
        downs.append(base + 2)
        slot, start = slot + 2, start + units
    for both, down in joined:
        base = len(weights)
        weights += [both, down]
        units = down.shape[0]
        copies += [(base, "column", slot, 0), (base + 1, "row", start, units)]
        pieces.append({"kind": "one", "slots": (slot,), "needs": (base,), "start": start, "units": units})
        downs.append(base + 1)
        slot, start = slot + 1, start + units
    columns = weights[0].shape[1]
    depth, model = weights[0].shape[0], weights[2].shape[1]
    row_starts, total = [], 0
    for block in blocks:
        row_starts.append(total)
        total += block.shape[0]
    plan = {
        "weights": len(weights),
        "copies": copies,
        "pieces": pieces,
        "downs": downs,
        "rows": row_starts,
        "width": width,
    }
    flops = 2 * total * depth * start * 3
    return pl.pallas_call(
        functools.partial(feed_forward_body, plan, len(blocks), weighted),
        in_specs=[pl.BlockSpec(memory_space=pltpu.VMEM) for _ in range(len(blocks) + 1)]
        + [pl.BlockSpec(memory_space=pl.ANY) for _ in weights],
        out_specs=[pl.BlockSpec(memory_space=pltpu.VMEM) for _ in blocks],
        out_shape=[jax.ShapeDtypeStruct((block.shape[0], model), kind) for block, kind in zip(blocks, out_types)],
        scratch_shapes=[
            pltpu.VMEM((slot, depth, columns), jnp.bfloat16),
            pltpu.VMEM((start, model), jnp.bfloat16),
            pltpu.VMEM((total, start), jnp.bfloat16),
            pltpu.SemaphoreType.DMA((len(copies),)),
        ],
        compiler_params=pltpu.CompilerParams(vmem_limit_bytes=48 * 1024 * 1024),
        cost_estimate=pl.CostEstimate(
            flops=flops, bytes_accessed=6 * depth * start + 4 * total * model, transcendentals=total * start
        ),
        name=name,
    )(*blocks, mask, *weights)


def attention(query_first, query_second, keys, head_count, lambda_head, head_gain):
    rows, width = query_first.shape
    size = width // head_count
    table = jnp.concatenate(keys, axis=0)
    values = table[:, 2 * width :]
    value_size = values.shape[1] // head_count
    outs = []
    for head in range(head_count):
        maps = []
        for number, query in enumerate((query_first, query_second)):
            q = query[:, head * size : (head + 1) * size]
            k = table[:, number * width + head * size : number * width + (head + 1) * size]
            scores = lax.dot_general(q, k, (((1,), (1,)), ((), ())), preferred_element_type=jnp.float32) * size**-0.5
            weights = jnp.exp(scores - jnp.max(scores, axis=-1, keepdims=True))
            total = jnp.sum(weights, axis=-1, keepdims=True)
            product = jnp.dot(
                weights.astype(jnp.bfloat16),
                values[:, head * value_size : (head + 1) * value_size],
                preferred_element_type=jnp.float32,
            )
            maps.append(product / total)
        mixture = maps[0] - lambda_head[head] * maps[1]
        outs.append(mixture * lax.rsqrt(jnp.mean(mixture * mixture, axis=-1, keepdims=True) + epsilon) * head_gain)
    return jnp.concatenate(outs, axis=1).astype(jnp.bfloat16)


def direct_shards(
    query_first,
    query_second,
    key_first,
    key_second,
    values,
    lambda_head,
    head_gain,
    out_weight,
    tokens,
    norm_gain,
    expert_ids,
    expert_weights,
    expert_gate,
    expert_up,
    expert_down,
    shared_gate,
    shared_up,
    shared_down,
):
    count, width_tp = lax.axis_size("ep"), lax.axis_size("tp")
    place, group = lax.axis_index("ep"), lax.axis_index("grp")
    heads_here = lambda_head.shape[0]
    row_count, model_width = tokens.shape
    gate, up, down = expert_gate[0], expert_up[0], expert_down[0]
    units = gate.shape[1]

    route = jnp.concatenate([expert_ids.astype(jnp.float32), expert_weights], axis=1)
    pair = prepare(tokens, swap_core(tokens), route, swap_core(route), norm_gain)

    sent = halves(gate, up, group)
    sent_down = lax.dynamic_slice_in_dim(down, group * (units // 2), units // 2, axis=0)
    near = swap_pair(sent)
    near_down = swap_pair(sent_down)
    far = swap_group(near)
    far_down = swap_group(near_down)

    def moved(value, step):
        return lax.ppermute(value, ("ep", "tp"), relay_pairs(count, width_tp, step))

    arrived = []
    latest = pair
    for step in range(1, count):
        latest = moved(latest, step)
        arrived.append(latest)

    kv_own = jnp.concatenate([key_first, key_second, values], axis=1)
    kv_pair = jnp.concatenate([kv_own, swap_core(kv_own)], axis=0)
    kv_rows = kv_own.shape[0]
    kv_mine, kv_other = [], []
    latest = kv_pair
    for step in range(1, count):
        latest = moved(latest, step)
        kv_mine.append(latest[:kv_rows])
        kv_other.append(swap_core(latest[kv_rows:]))
    kv_blocks = [kv_own]
    for step in range(1, count):
        kv_blocks.append(kv_mine[step - 1] + kv_other[count - step - 1])

    lanes = jnp.arange(lane_count, dtype=jnp.int32)
    mask = jnp.where((lanes % third == place) & (lanes < 3 * third), 1.0, 0.0).astype(jnp.float32)[None]
    pairs = [(gate, up, down), (swap_core(gate), swap_core(up), swap_core(down))]
    joined = [
        (near, near_down),
        (swap_core(near), swap_core(near_down)),
        (far, far_down),
        (swap_core(far), swap_core(far_down)),
    ]
    (last,) = feed_forward([arrived[-1]], mask, pairs, joined, True, [jnp.bfloat16], model_width, "routed_far")
    rest_blocks = list(reversed(arrived[:-1])) + [pair[:row_count]]
    rest = feed_forward(
        rest_blocks,
        mask,
        pairs,
        joined,
        True,
        [jnp.bfloat16] * (count - 2) + [jnp.float32],
        model_width,
        "routed_near",
    )
    partial = [last] + list(rest)
    running = last
    for step in range(1, count):
        running = lax.ppermute(running, ("ep", "tp"), return_pairs(count, width_tp, step))
        if step < count - 1:
            running = (running.astype(jnp.float32) + partial[step].astype(jnp.float32)).astype(jnp.bfloat16)

    shared_own = (shared_gate, shared_up, shared_down)
    shared_near = tuple(swap_pair(piece) for piece in shared_own)
    shared_pieces = [
        shared_own,
        tuple(swap_core(piece) for piece in shared_own),
        shared_near,
        tuple(swap_core(piece) for piece in shared_near),
    ]
    (shared_out,) = feed_forward(
        [pair[:row_count]], mask, shared_pieces, [], False, [jnp.float32], model_width, "shared"
    )

    head_local = attention(query_first, query_second, kv_blocks, heads_here, lambda_head, head_gain)
    position_heads = lax.all_to_all(head_local, "tp", split_axis=0, concat_axis=1, tiled=True)
    mixed = jnp.dot(position_heads, out_weight, preferred_element_type=jnp.float32).astype(jnp.bfloat16)

    other_half = swap_core(running[row_count:])
    expert_out = (
        rest[-1] + shared_out + running[:row_count].astype(jnp.float32) + other_half.astype(jnp.float32)
    ).astype(jnp.bfloat16)
    return (mixed, expert_out)


def shards(
    query_first,
    query_second,
    key_first,
    key_second,
    values,
    lambda_head,
    head_gain,
    out_weight,
    tokens,
    norm_gain,
    expert_ids,
    expert_weights,
    expert_gate,
    expert_up,
    expert_down,
    shared_gate,
    shared_up,
    shared_down,
):
    shard_rows, query_width = query_first.shape
    heads_here = lambda_head.shape[0]
    head_size = query_width // heads_here
    value_size = values.shape[1] // heads_here
    score_scale = head_size ** (-0.5)
    query_one = query_first.reshape(shard_rows, heads_here, head_size)
    query_two = query_second.reshape(shard_rows, heads_here, head_size)
    initial = (
        jnp.full((shard_rows, heads_here), -jnp.inf, jnp.float32),
        jnp.zeros((shard_rows, heads_here), jnp.float32),
        jnp.zeros((shard_rows, heads_here, value_size), jnp.float32),
    )
    carried = (initial, initial)
    key_one = lax.all_gather(key_first, "ep", axis=0, tiled=True)
    key_two = lax.all_gather(key_second, "ep", axis=0, tiled=True)
    value_piece = lax.all_gather(values, "ep", axis=0, tiled=True)
    total_rows = key_one.shape[0]
    block_rows = key_block(total_rows, shard_rows)
    block_count = total_rows // block_rows
    stacked = (
        key_one.reshape(block_count, block_rows, heads_here, head_size),
        key_two.reshape(block_count, block_rows, heads_here, head_size),
        value_piece.reshape(block_count, block_rows, heads_here, value_size),
    )

    def fold_step(states, blocks):
        first_state, second_state = states
        key_a, key_b, value_block = blocks
        scores_a = (
            jnp.einsum("qhd,khd->qhk", query_one, key_a, preferred_element_type=jnp.float32)
            * score_scale
        )
        scores_b = (
            jnp.einsum("qhd,khd->qhk", query_two, key_b, preferred_element_type=jnp.float32)
            * score_scale
        )
        return (
            (
                softmax_update(first_state, scores_a, value_block),
                softmax_update(second_state, scores_b, value_block),
            ),
            None,
        )

    carried, unused = lax.scan(fold_step, carried, stacked)
    first_state, second_state = carried
    first_out = first_state[2] / first_state[1][..., None]
    second_out = second_state[2] / second_state[1][..., None]
    mixture = first_out - lambda_head[None, :, None] * second_out
    normed_heads = (
        mixture
        * lax.rsqrt(jnp.mean(mixture * mixture, axis=-1, keepdims=True) + epsilon)
        * head_gain
    )
    head_local = normed_heads.astype(jnp.bfloat16).reshape(shard_rows, heads_here * value_size)
    position_heads = lax.all_to_all(head_local, "tp", split_axis=0, concat_axis=1, tiled=True)
    mixed = jnp.dot(position_heads, out_weight, preferred_element_type=jnp.float32).astype(
        jnp.bfloat16
    )
    row_count, model_width = tokens.shape
    top_count = expert_ids.shape[1]
    ep_count = lax.axis_size("ep")
    local_experts = expert_gate.shape[0]
    expert_count = local_experts * ep_count
    capacity = max(2, row_count * top_count * 3 // (2 * expert_count))
    routed_rows = expert_count * capacity
    owner_span = routed_rows + row_count
    widened = tokens.astype(jnp.float32)
    normed = (
        widened
        * lax.rsqrt(jnp.mean(widened * widened, axis=-1, keepdims=True) + epsilon)
        * norm_gain
    ).astype(jnp.bfloat16)
    flat_ids = expert_ids.reshape(-1)
    onehot = (flat_ids[:, None] == jnp.arange(expert_count, dtype=jnp.int32)[None, :]).astype(
        jnp.int32
    )
    ranks = jnp.sum(onehot * jnp.cumsum(onehot, axis=0), axis=1) - 1
    slot_index = flat_ids * capacity + ranks
    token_index = jnp.arange(flat_ids.shape[0], dtype=jnp.int32) // top_count
    filled = jnp.full((routed_rows,), row_count, jnp.int32).at[slot_index].set(token_index)
    padded = jnp.concatenate([normed, jnp.zeros((1, model_width), jnp.bfloat16)], axis=0)
    outgoing = padded[filled].reshape(1, ep_count, local_experts * capacity, model_width)
    arrived = lax.all_to_all(outgoing, "ep", split_axis=1, concat_axis=1, tiled=True)
    local_rows = jnp.concatenate(
        [arrived.reshape(1, routed_rows, model_width), normed[None]], axis=1
    )
    gathered = lax.all_gather(local_rows, "tp", axis=0, tiled=True)
    owners = owner_span * lax.axis_size("tp") // owner_span
    routed_in = gathered[:, :routed_rows].reshape(
        owners, ep_count, local_experts, capacity, model_width
    )
    gate_value = jnp.einsum(
        "osecd,edf->osecf", routed_in, expert_gate, preferred_element_type=jnp.float32
    )
    up_value = jnp.einsum(
        "osecd,edf->osecf", routed_in, expert_up, preferred_element_type=jnp.float32
    )
    hidden = (jax.nn.silu(gate_value) * up_value).astype(jnp.bfloat16)
    routed_out = jnp.einsum(
        "osecf,efd->osecd", hidden, expert_down, preferred_element_type=jnp.float32
    )
    routed_out = routed_out.reshape(owners, routed_rows, model_width)
    shared_in = gathered[:, routed_rows:]
    shared_gate_value = jnp.einsum(
        "ord,df->orf", shared_in, shared_gate, preferred_element_type=jnp.float32
    )
    shared_up_value = jnp.einsum(
        "ord,df->orf", shared_in, shared_up, preferred_element_type=jnp.float32
    )
    shared_hidden = (jax.nn.silu(shared_gate_value) * shared_up_value).astype(jnp.bfloat16)
    shared_out = jnp.einsum(
        "orf,fd->ord", shared_hidden, shared_down, preferred_element_type=jnp.float32
    )
    kept_rows = lax.psum_scatter(
        jnp.concatenate([routed_out, shared_out], axis=1)
        .reshape(owners * owner_span, model_width)
        .astype(jnp.bfloat16),
        "tp",
        scatter_dimension=0,
        tiled=True,
    ).astype(jnp.float32)
    routed_back = (
        kept_rows[:routed_rows]
        .astype(jnp.bfloat16)
        .reshape(ep_count, local_experts * capacity, model_width)
    )
    returned = lax.all_to_all(routed_back, "ep", split_axis=0, concat_axis=0, tiled=True).reshape(
        routed_rows, model_width
    )
    picked = returned[slot_index].reshape(row_count, top_count, model_width).astype(jnp.float32)
    combined = jnp.sum(picked * expert_weights[:, :, None], axis=1) + kept_rows[routed_rows:]
    expert_out = combined.astype(jnp.bfloat16)
    return (mixed, expert_out)


def solution(mesh):
    placed = (
        P(("grp", "ep"), "tp"),
        P(("grp", "ep"), "tp"),
        P(("grp", "ep"), "tp"),
        P(("grp", "ep"), "tp"),
        P(("grp", "ep"), "tp"),
        P("tp"),
        P(),
        P(),
        P(("grp", "ep", "tp"), None),
        P(),
        P(("grp", "ep", "tp"), None),
        P(("grp", "ep", "tp"), None),
        P("ep", None, "tp"),
        P("ep", None, "tp"),
        P("ep", "tp", None),
        P(None, "tp"),
        P(None, "tp"),
        P("tp", None),
    )
    sizes = dict(mesh.shape)

    def chosen(*arrays):
        experts = arrays[12].shape[0]
        direct = (
            sizes["grp"] == 2
            and sizes["tp"] == 4
            and sizes["ep"] == experts
            and 3 <= experts <= 8
        )
        body = direct_shards if direct else shards
        return mapped(body)(*arrays)

    def mapped(body):
        return jax.shard_map(
            body,
            mesh=mesh,
            in_specs=placed,
            out_specs=(P(("grp", "ep", "tp"), None), P(("grp", "ep", "tp"), None)),
            check_vma=False,
        )

    return chosen
```
